32 devices in a mesh: dp: 4 (over y, x), kv: 4 (over z), tp: 2 (over core).
Axes of the slice: x: 2, y: 2, z: 4, core: 2. Of those that a mesh axis runs over, the one named last changes fastest.
Arguments:
- tokens: bfloat16 [4096, 2048], P(('dp', 'kv'), 'tp'), parts along dimension 0, may hold values from -6 to 6
- query_weight: bfloat16 [2048, 1024], P(None, 'tp'), may hold values from -2 to 2
- key_weight: bfloat16 [2048, 1024], P(None, 'tp'), may hold values from -2 to 2
- value_weight: bfloat16 [2048, 1024], P(None, 'tp'), may hold values from -0.125 to 0.125
- out_weight: bfloat16 [1024, 2048], P(None, 'tp'), may hold values from -0.75 to 0.75
- chosen: int32 [128, 16], P(('dp', 'kv')), parts along dimension 0, may hold values from -1 to 31, as said below
Outputs:
- mixed: bfloat16 [4096, 2048], P(('dp', 'kv'), 'tp'), parts along dimension 0
The draws below stay inside these ranges and needn't reach their ends.
There are 4 independent parts, one for each index of `dp`. The reference program is written for one: setup_inputs(seed, part) draws one part's arguments, and reference() takes and returns one part's arrays. A program takes and returns all parts, laid end to end along the dimension named above; an argument that names none is the same for every part. Nothing has to cross between parts.
Inputs may be any that keep to these rules, and one draw needn't show every extreme that they name: Each row of chosen lists distinct key blocks no later than its own query block, followed or mixed with -1 for empty slots; the own block is always listed, and block 0 too. For the 8 query blocks of one index of kv (aligned runs of rows), the distinct listed key blocks that lie among the 8 blocks of any one other index number at most 3, and exactly 3 for the index just before.
All inputs are finite; a program needn't handle non-finite values.
Results may differ from the reference program's by a relative error of at most 0.0084.
Values may be sent and summed in bfloat16 or wider, within the bound.
No kernel may reach another device: no remote copies, remote signals or barrier semaphores. Data moves between devices by JAX's collectives and lax.ppermute only.
A program may use at most 128 MiB of HBM per device.

```python
import jax
import jax.numpy as jnp
from jax import lax

D = 2048
HEADS = 16
HEAD_DIM = 64
BLOCK = 32
TOPK = 16
CAP = 3
HW = 1024
BLK_DEV = 8
LEN = 1024
NBLK = 32


def paired_weights(key):
    first_key, second_key = jax.random.split(jax.random.fold_in(key, 5), 2)
    fan_scale = D ** (-0.5)
    base_draw = jax.random.normal(first_key, (D, HW), jnp.float32)
    other_draw = jax.random.normal(second_key, (D, HW), jnp.float32)
    query_part = base_draw
    key_part = other_draw
    return (jnp.clip(query_part * fan_scale, -2.0, 2.0), jnp.clip(key_part * fan_scale, -2.0, 2.0))


def draw_query_weight(key, part):
    return paired_weights(key)[0].astype(jnp.bfloat16)


def draw_key_weight(key, part):
    return paired_weights(key)[1].astype(jnp.bfloat16)


def draw_chosen(key, part):
    devices = NBLK // BLK_DEV
    key_popular, key_pick, key_score = jax.random.split(jax.random.fold_in(key, 11), 3)
    block_ids = jnp.arange(NBLK, dtype=jnp.int32)
    owner = block_ids // BLK_DEV
    local_index = block_ids % BLK_DEV
    popular = (jax.random.randint(key_popular, (NBLK,), 0, 8) == 0).astype(jnp.int32)
    asker = jnp.arange(devices, dtype=jnp.int32)[:, None]
    pick_score = jax.random.randint(key_pick, (devices, NBLK), 0, 4096) + popular[None, :] * 8192
    forced = (owner[None, :] == asker - 1) & (local_index[None, :] == BLK_DEV - 1) | (block_ids[None, :] == 0)
    pick_score = jnp.where(forced, 16384, pick_score) * BLK_DEV + (BLK_DEV - 1 - local_index)[None, :]
    pick_grid = pick_score.reshape(devices, devices, BLK_DEV)
    rank_in = jnp.sum((pick_grid[..., None, :] > pick_grid[..., :, None]).astype(jnp.int32), axis=-1)
    holder_ids = jnp.arange(devices, dtype=jnp.int32)
    allowed = (rank_in < CAP) & (holder_ids[None, :, None] < asker[:, :, None])
    allowed = allowed.reshape(devices, NBLK)
    query_block = block_ids[:, None]
    key_block = block_ids[None, :]
    query_owner = query_block // BLK_DEV
    local_ok = (key_block // BLK_DEV == query_owner) & (key_block <= query_block)
    remote_ok = allowed[query_owner[:, 0]]
    valid = local_ok | remote_ok
    mandatory = (key_block == query_block) | remote_ok & (key_block // BLK_DEV == query_owner - 1)
    mandatory = mandatory | (key_block == 0) & valid
    noise = jax.random.randint(key_score, (NBLK, NBLK), 0, 4096) + popular[None, :] * 4096
    score_int = jnp.where(mandatory, 16384, noise)
    score_int = jnp.where(valid, score_int * NBLK + key_block, -1)
    top_values, top_index = lax.top_k(score_int, TOPK)
    return jnp.where(top_values >= 0, top_index, -1).astype(jnp.int32)


def levels(own_key, shape, cuts, low, top_value):
    loudness, own = 1.0, jax.random.fold_in(own_key, 6)
    for position, parts in cuts:
        steps = jnp.exp(jax.random.uniform(jax.random.fold_in(own, position), (parts,), jnp.float32, low / len(cuts), top_value / len(cuts)))
        loudness = loudness * jnp.repeat(steps, shape[position] // parts).reshape([-1 if axis == position else 1 for axis in range(len(shape))])
    return loudness


def centred(rng, shape, spread, reach, cuts=(), kind=jnp.bfloat16):
    result = spread * jax.random.normal(rng, shape, jnp.float32)
    if cuts:
        result = result * levels(rng, shape, cuts, -0.22, 0.18)
    return jnp.clip(result, -reach, reach).astype(kind)


def setup_inputs(seed: int = 0, part: int = 0) -> dict:
    arg_keys = jax.random.split(jax.random.key(seed), 7)
    part_keys = jax.random.split(jax.random.fold_in(arg_keys[6], part), 7)
    return {
        "tokens": centred(part_keys[0], (LEN, D), 1.0, 6.0, ((0, 4), (1, 2))),
        "query_weight": draw_query_weight(jax.random.fold_in(arg_keys[6], 71), part),
        "key_weight": draw_key_weight(jax.random.fold_in(arg_keys[6], 71), part),
        "value_weight": centred(arg_keys[3], (D, HW), D ** -0.5, 0.125, ((1, 2),)),
        "out_weight": centred(arg_keys[4], (HW, D), (HW // 16) ** -0.5, 0.75, ((1, 2),)),
        "chosen": draw_chosen(jax.random.fold_in(jax.random.fold_in(arg_keys[6], part), 71), part),
    }


rotary_base = 500000.0
masked_score = -1e30


def rotate(heads_in, positions):
    half_dim = heads_in.shape[-1] // 2
    inverse = 1.0 / (rotary_base ** (jnp.arange(half_dim, dtype=jnp.float32) / half_dim))
    angles = positions.astype(jnp.float32)[:, None] * inverse[None, :]
    cosine = jnp.cos(angles)[:, None, :]
    sine_part = jnp.sin(angles)[:, None, :]
    first_half = heads_in[..., :half_dim]
    second_half = heads_in[..., half_dim:]
    return jnp.concatenate([first_half * cosine - second_half * sine_part,
                            first_half * sine_part + second_half * cosine], axis=-1)


def reference(tokens, query_weight, key_weight, value_weight, out_weight, chosen):
    length = tokens.shape[0]
    positions = jnp.arange(length, dtype=jnp.int32)
    heads_shape = (length, HEADS, HEAD_DIM)
    query_proj = rotate(jnp.dot(tokens, query_weight, preferred_element_type=jnp.float32).reshape(heads_shape),
                        positions).astype(jnp.bfloat16)
    key_proj = rotate(jnp.dot(tokens, key_weight, preferred_element_type=jnp.float32).reshape(heads_shape),
                      positions).astype(jnp.bfloat16)
    value_proj = jnp.dot(tokens, value_weight, preferred_element_type=jnp.float32).astype(jnp.bfloat16).reshape(heads_shape)
    blocks = length // BLOCK
    key_blocks = key_proj.reshape(blocks, BLOCK, HEADS, HEAD_DIM)
    value_blocks = value_proj.reshape(blocks, BLOCK, HEADS, HEAD_DIM)
    query_blocks = query_proj.reshape(blocks, BLOCK, HEADS, HEAD_DIM)
    score_scale = HEAD_DIM ** -0.5

    def one_block(inputs):
        query_block, listed, block_index = inputs
        safe_index = jnp.maximum(listed, 0).astype(jnp.int32)
        keys_sel = key_blocks[safe_index].reshape(TOPK * BLOCK, HEADS, HEAD_DIM).astype(jnp.float32)
        values_sel = value_blocks[safe_index].reshape(TOPK * BLOCK, HEADS, HEAD_DIM).astype(jnp.float32)
        key_pos = (safe_index[:, None] * BLOCK + jnp.arange(BLOCK, dtype=jnp.int32)[None, :]).reshape(-1)
        key_valid = jnp.repeat(listed >= 0, BLOCK)
        query_pos = block_index * BLOCK + jnp.arange(BLOCK, dtype=jnp.int32)
        allowed = key_valid[None, :] & (key_pos[None, :] <= query_pos[:, None])
        scores = jnp.einsum("qhd,khd->hqk", query_block.astype(jnp.float32), keys_sel) * score_scale
        scores = jnp.where(allowed[None], scores, masked_score)
        peak_row = jnp.max(scores, axis=2, keepdims=True)
        weights = jnp.where(allowed[None], jnp.exp(scores - peak_row), 0.0)
        denominator = jnp.sum(weights, axis=2)
        weight_low = lax.optimization_barrier(weights.astype(jnp.bfloat16))
        summed = jnp.einsum("hqk,khd->qhd", weight_low.astype(jnp.float32), values_sel)
        return (summed / denominator.T[:, :, None]).astype(jnp.bfloat16)

    attended = lax.map(one_block, (query_blocks, chosen, jnp.arange(blocks, dtype=jnp.int32)))
    attended = attended.reshape(length, HEADS * HEAD_DIM)
    return jnp.dot(attended, out_weight, preferred_element_type=jnp.float32).astype(jnp.bfloat16)
```

```python
import functools

import jax
import jax.numpy as jnp
from jax import lax
from jax.experimental import pallas as pl
from jax.experimental.pallas import tpu as pltpu
from jax.sharding import PartitionSpec as P

HEAD_DIM = 64
BLOCK = 32
CAP = 3
LANES = 128

rotary_base = 500000.0
masked_score = -1e30
score_factor = HEAD_DIM ** (-0.5) * 1.4426950408889634


VMEM = pl.BlockSpec(memory_space=pltpu.VMEM)


def rotary_tables(first_pos, rows):
    half = HEAD_DIM // 2
    lane = jnp.arange(LANES, dtype=jnp.int32)
    inverse = 1.0 / rotary_base ** (jnp.arange(half, dtype=jnp.float32) / half)
    inverse = jnp.tile(inverse, LANES // half)
    positions = first_pos + jnp.arange(rows, dtype=jnp.int32)
    angles = positions.astype(jnp.float32)[:, None] * inverse[None, :]
    sign = jnp.where(lane % HEAD_DIM < half, -1.0, 1.0)
    return jnp.cos(angles), jnp.sin(angles) * sign[None, :]


def rotate(acc, cosine, sine):
    half = HEAD_DIM // 2
    lane = lax.broadcasted_iota(jnp.int32, (acc.shape[0], LANES), 1)
    first = lane % HEAD_DIM < half
    out = []
    for start in range(0, acc.shape[1], LANES):
        part = acc[:, start : start + LANES]
        partner = jnp.where(
            first, pltpu.roll(part, LANES - half, 1), pltpu.roll(part, half, 1)
        )
        out.append(part * cosine + partner * sine)
    return jnp.concatenate(out, axis=1)


def project(own_ref, other_ref, weight_ref):
    mine = lax.axis_index("tp")
    depth = own_ref.shape[1]
    own_rows = pl.ds(pl.multiple_of(mine * depth, depth), depth)
    other_rows = pl.ds(pl.multiple_of((1 - mine) * depth, depth), depth)
    return jnp.dot(
        own_ref[...], weight_ref[own_rows, :], preferred_element_type=jnp.float32
    ) + jnp.dot(
        other_ref[...], weight_ref[other_rows, :], preferred_element_type=jnp.float32
    )


def key_value_kernel(own_ref, other_ref, key_ref, value_ref, cos_ref, sin_ref, out_ref):
    step = pl.program_id(0)
    half = pl.num_programs(0) // 2

    @pl.when(step < half)
    def _():
        acc = project(own_ref, other_ref, key_ref)
        out_ref[...] = rotate(acc, cos_ref[...], sin_ref[...]).astype(jnp.bfloat16)

    @pl.when(step >= half)
    def _():
        out_ref[...] = project(own_ref, other_ref, value_ref).astype(jnp.bfloat16)


def query_kernel(own_ref, other_ref, weight_ref, cos_ref, sin_ref, out_ref):
    acc = project(own_ref, other_ref, weight_ref)
    out_ref[...] = rotate(acc, cos_ref[...], sin_ref[...]).astype(jnp.bfloat16)


def key_value(own, other, key_weight, value_weight, cosine, sine):
    rows, depth = own.shape
    width = key_weight.shape[1]
    tile = 256
    steps = width // tile
    whole = pl.BlockSpec((rows, depth), lambda i: (0, 0))
    table = pl.BlockSpec((rows, LANES), lambda i: (0, 0))
    return pl.pallas_call(
        key_value_kernel,
        grid=(2 * steps,),
        in_specs=[
            whole,
            whole,
            pl.BlockSpec((2 * depth, tile), lambda i: (0, jnp.minimum(i, steps - 1))),
            pl.BlockSpec((2 * depth, tile), lambda i: (0, jnp.maximum(i - steps, 0))),
            table,
            table,
        ],
        out_specs=pl.BlockSpec((rows, tile), lambda i: (0, i)),
        out_shape=jax.ShapeDtypeStruct((rows, 2 * width), jnp.bfloat16),
        cost_estimate=pl.CostEstimate(
            flops=8 * rows * depth * width, bytes_accessed=8 * depth * width, transcendentals=0
        ),
        name="key_value",
    )(own, other, key_weight, value_weight, cosine, sine)


def query(own, other, weight, cosine, sine):
    rows, depth = own.shape
    width = weight.shape[1]
    tile = 256
    whole = pl.BlockSpec((rows, depth), lambda i: (0, 0))
    table = pl.BlockSpec((rows, LANES), lambda i: (0, 0))
    return pl.pallas_call(
        query_kernel,
        grid=(width // tile,),
        in_specs=[whole, whole, pl.BlockSpec((2 * depth, tile), lambda i: (0, i)), table, table],
        out_specs=pl.BlockSpec((rows, tile), lambda i: (0, i)),
        out_shape=jax.ShapeDtypeStruct((rows, width), jnp.bfloat16),
        cost_estimate=pl.CostEstimate(
            flops=4 * rows * depth * width, bytes_accessed=4 * depth * width, transcendentals=0
        ),
        name="query",
    )(own, other, weight, cosine, sine)


def pick_kernel(asked_ref, store_ref, out_ref):
    blocks = store_ref.shape[0] // BLOCK
    first = lax.axis_index("kv") * blocks
    asked = asked_ref[...]
    count = jnp.int32(0)
    index = [jnp.int32(0)] * CAP
    for block in range(blocks):
        hit = jnp.max((asked == first + block).astype(jnp.int32))
        for slot in range(CAP):
            index[slot] = jnp.where((hit == 1) & (count == slot), block, index[slot])
        count = count + hit
    for slot in range(CAP):
        rows = pl.ds(pl.multiple_of(index[slot] * BLOCK, BLOCK), BLOCK)
        out_ref[slot * BLOCK : (slot + 1) * BLOCK, :] = store_ref[rows, :]


def pick(asked, store):
    return pl.pallas_call(
        pick_kernel,
        in_specs=[VMEM, VMEM],
        out_specs=VMEM,
        out_shape=jax.ShapeDtypeStruct((CAP * BLOCK, store.shape[1]), store.dtype),
        cost_estimate=pl.CostEstimate(flops=100000, bytes_accessed=400000, transcendentals=0),
        name="pick",
    )(asked, store)


def head_pair_queries(queries):
    lane = lax.broadcasted_iota(jnp.int32, queries.shape, 1)
    zero = jnp.zeros_like(queries)
    return jnp.concatenate(
        [jnp.where(lane < HEAD_DIM, queries, zero), jnp.where(lane < HEAD_DIM, zero, queries)],
        axis=0,
    )


def pair_scores(keys, queries):
    return lax.dot_general(
        keys, queries, (((1,), (1,)), ((), ())), preferred_element_type=jnp.float32
    )


def pair_values(values, weights):
    both = lax.dot_general(
        values, weights, (((0,), (0,)), ((), ())), preferred_element_type=jnp.float32
    )
    rows = weights.shape[1] // 2
    return jnp.concatenate([both[:HEAD_DIM, :rows], both[HEAD_DIM:, rows:]], axis=0)


def widen(stat):
    rows = stat.shape[1] // 2
    return jnp.concatenate(
        [
            jnp.broadcast_to(stat[:, :rows], (HEAD_DIM, rows)),
            jnp.broadcast_to(stat[:, rows:], (HEAD_DIM, rows)),
        ],
        axis=0,
    )


def local_kernel(query_ref, store_ref, bias_ref, peak_ref, total_ref, summed_ref):
    rows = query_ref.shape[0]
    width = query_ref.shape[1]
    blocks = rows // BLOCK
    listed = jnp.concatenate(
        [jnp.broadcast_to(bias_ref[b : b + 1, :], (BLOCK, rows)) for b in range(blocks)], axis=0
    )
    key_row = lax.broadcasted_iota(jnp.int32, (rows, rows), 0)
    query_row = lax.broadcasted_iota(jnp.int32, (rows, rows), 1)
    bias = jnp.where(key_row <= query_row, listed, masked_score)
    bias = jnp.concatenate([bias, bias], axis=1)
    for pair in range(width // LANES):
        lanes = slice(pair * LANES, (pair + 1) * LANES)
        queries = head_pair_queries(query_ref[:, lanes])
        scores = pair_scores(store_ref[:, lanes], queries) + bias
        peak = jnp.max(scores, axis=0, keepdims=True)
        weights = jnp.exp2((scores - peak) * score_factor)
        peak_ref[pair : pair + 1, :] = peak
        total_ref[pair : pair + 1, :] = jnp.sum(weights, axis=0, keepdims=True)
        values = store_ref[:, width + pair * LANES : width + (pair + 1) * LANES]
        summed_ref[lanes, :] = pair_values(values, weights.astype(jnp.bfloat16))


def local_attention(queries, store, bias):
    rows, width = queries.shape
    pairs = width // LANES
    return pl.pallas_call(
        local_kernel,
        in_specs=[VMEM] * 3,
        out_specs=[VMEM] * 3,
        out_shape=[
            jax.ShapeDtypeStruct((pairs, 2 * rows), jnp.float32),
            jax.ShapeDtypeStruct((pairs, 2 * rows), jnp.float32),
            jax.ShapeDtypeStruct((width, rows), jnp.float32),
        ],
        cost_estimate=pl.CostEstimate(
            flops=16 * rows * rows * width, bytes_accessed=2000000, transcendentals=0
        ),
        name="local_attention",
    )(queries, store, bias)


def remote_kernel(shifts, query_ref, bias_ref, peak_ref, total_ref, summed_ref, *refs):
    got_refs, out_ref = refs[:shifts], refs[shifts]
    rows, width = query_ref.shape
    for pair in range(width // LANES):
        lanes = slice(pair * LANES, (pair + 1) * LANES)
        queries = head_pair_queries(query_ref[:, lanes])
        peak = peak_ref[pair : pair + 1, :]
        total = total_ref[pair : pair + 1, :]
        summed = summed_ref[lanes, :]
        for shift in range(shifts):
            got = got_refs[shift]
            scores = pair_scores(got[:, lanes], queries)
            bias = jnp.concatenate(
                [
                    jnp.broadcast_to(
                        bias_ref[shift * CAP + slot : shift * CAP + slot + 1, :], (BLOCK, rows)
                    )
                    for slot in range(CAP)
                ],
                axis=0,
            )
            scores = scores + jnp.concatenate([bias, bias], axis=1)
            peak_new = jnp.maximum(peak, jnp.max(scores, axis=0, keepdims=True))
            factor = jnp.exp2((peak - peak_new) * score_factor)
            weights = jnp.exp2((scores - peak_new) * score_factor)
            total = total * factor + jnp.sum(weights, axis=0, keepdims=True)
            values = got[:, width + pair * LANES : width + (pair + 1) * LANES]
            summed = summed * widen(factor) + pair_values(values, weights.astype(jnp.bfloat16))
            peak = peak_new
        attended = summed / widen(total)
        out_ref[:, lanes] = attended.T.astype(jnp.bfloat16)


def remote_attention(queries, bias, state, got):
    rows, width = queries.shape
    shifts = len(got)
    return pl.pallas_call(
        functools.partial(remote_kernel, shifts),
        in_specs=[VMEM] * (5 + shifts),
        out_specs=VMEM,
        out_shape=jax.ShapeDtypeStruct((rows, width), jnp.bfloat16),
        cost_estimate=pl.CostEstimate(
            flops=16 * rows * CAP * BLOCK * shifts * width, bytes_accessed=2000000, transcendentals=0
        ),
        name="remote_attention",
    )(queries, bias, *state, *got)


def out_kernel(own_ref, other_ref, weight_ref, out_ref):
    out_ref[...] = project(own_ref, other_ref, weight_ref).astype(jnp.bfloat16)


def out_projection(own, other, weight):
    rows, depth = own.shape
    width = weight.shape[1]
    tile = 256
    whole = pl.BlockSpec((rows, depth), lambda i: (0, 0))
    return pl.pallas_call(
        out_kernel,
        grid=(width // tile,),
        in_specs=[whole, whole, pl.BlockSpec((2 * depth, tile), lambda i: (0, i))],
        out_specs=pl.BlockSpec((rows, tile), lambda i: (0, i)),
        out_shape=jax.ShapeDtypeStruct((rows, width), jnp.bfloat16),
        name="out_projection",
    )(own, other, weight)


def bias_rows(hit, rows):
    bias = jnp.where(hit, 0.0, masked_score).astype(jnp.float32)
    return jnp.broadcast_to(bias[:, :, None], (*bias.shape, BLOCK)).reshape(bias.shape[0], rows)


def listed_bias(chosen, device, devices, rows):
    blocks = rows // BLOCK
    shift = jnp.arange(devices, dtype=jnp.int32)
    source = device - shift
    ids = source[:, None] * blocks + jnp.arange(blocks, dtype=jnp.int32)[None, :]
    listed = jnp.any(chosen[None, None, :, :] == ids[:, :, None, None], axis=3)
    listed = listed & (source >= 0)[:, None, None]
    needed = jnp.any(listed, axis=2)
    earlier = jnp.arange(blocks)[:, None] > jnp.arange(blocks)[None, :]
    rank = jnp.sum(jnp.where(earlier[None] & needed[:, None, :], 1, 0), axis=2)
    slot = jnp.arange(CAP, dtype=jnp.int32)
    slot_hit = needed[:, None, :] & (rank[:, None, :] == slot[None, :, None])
    hit = jnp.any(slot_hit[:, :, :, None] & listed[:, None, :, :], axis=2)
    return bias_rows(listed[0], rows), bias_rows(hit[1:].reshape(-1, blocks), rows)


def on_device(tokens, query_weight, key_weight, value_weight, out_weight, chosen):
    rows = tokens.shape[0]
    device = lax.axis_index("kv")
    devices = lax.axis_size("kv")
    swap = [(0, 1), (1, 0)]
    other = lax.ppermute(tokens, "tp", swap)
    asked = [
        lax.ppermute(chosen, "kv", [(i, i - k) for i in range(k, devices)])
        for k in range(1, devices)
    ]
    cosine, sine = rotary_tables(device * rows, rows)
    store = key_value(tokens, other, key_weight, value_weight, cosine, sine)
    got = [
        lax.ppermute(pick(asked[k - 1], store), "kv", [(i, i + k) for i in range(devices - k)])
        for k in range(1, devices)
    ]
    queries = query(tokens, other, query_weight, cosine, sine)
    local_bias, remote_bias = listed_bias(chosen, device, devices, rows)
    state = local_attention(queries, store, local_bias)
    attended = remote_attention(queries, remote_bias, state, got)
    attended_other = lax.ppermute(attended, "tp", swap)
    return out_projection(attended, attended_other, out_weight)


def solution(mesh):
    placed = (
        P(("dp", "kv"), "tp"),
        P(None, "tp"),
        P(None, "tp"),
        P(None, "tp"),
        P(None, "tp"),
        P(("dp", "kv"), None),
    )
    return jax.shard_map(
        on_device, mesh=mesh, in_specs=placed, out_specs=P(("dp", "kv"), "tp"), check_vma=False
    )
```

```python
import functools

import jax
import jax.numpy as jnp
from jax import lax
from jax.experimental import pallas as pl
from jax.experimental.pallas import tpu as pltpu
from jax.sharding import PartitionSpec as P


HEAD_DIM = 64
BLOCK = 32
CAP = 3
LANES = 128

rotary_base = 500000.0
masked_score = -1e30
score_factor = HEAD_DIM ** (-0.5) * 1.4426950408889634


VMEM = pl.BlockSpec(memory_space=pltpu.VMEM)


def call(kernel, operands, results, flops=1000000, limit=16, scratch=(), far=0):
    anywhere = pl.BlockSpec(memory_space=pl.ANY)
    near = len(operands) - far
    out = pl.pallas_call(
        kernel,
        in_specs=[VMEM] * near + [anywhere] * far,
        out_specs=[anywhere if r.memory_space == pltpu.HBM else VMEM for r in results],
        out_shape=results,
        scratch_shapes=list(scratch),
        cost_estimate=pl.CostEstimate(flops=flops, bytes_accessed=100000, transcendentals=0),
        compiler_params=pltpu.CompilerParams(vmem_limit_bytes=limit << 20),
    )(
        *[pltpu.with_memory_space_constraint(x, pltpu.VMEM) for x in operands[:near]],
        *[pltpu.with_memory_space_constraint(x, pltpu.HBM) for x in operands[near:]],
    )
    return out[0] if len(results) == 1 else out


def dot(left, right):
    return jnp.dot(left, right, preferred_element_type=jnp.float32)


def table_kernel(angle_ref, cos_ref, sin_ref):
    blocks = cos_ref.shape[0] // BLOCK
    cosine, sine = jnp.cos(angle_ref[...]), jnp.sin(angle_ref[...])
    lane = lax.broadcasted_iota(jnp.int32, (BLOCK, LANES), 1)
    sign = jnp.where(lane % HEAD_DIM < HEAD_DIM // 2, -1.0, 1.0)
    cos_in, sin_in = cosine[:BLOCK], sine[:BLOCK]
    for block in range(blocks):
        rows = slice(block * BLOCK, (block + 1) * BLOCK)
        cos_at = cosine[BLOCK + block : BLOCK + block + 1]
        sin_at = sine[BLOCK + block : BLOCK + block + 1]
        cos_ref[rows, :] = cos_in * cos_at - sin_in * sin_at
        sin_ref[rows, :] = (sin_in * cos_at + cos_in * sin_at) * sign


def rotary_tables(first_pos, rows):
    half = HEAD_DIM // 2
    inverse = 1.0 / rotary_base ** (jnp.arange(half, dtype=jnp.float32) / half)
    inverse = jnp.tile(inverse, LANES // half)
    offsets = jnp.arange(BLOCK, dtype=jnp.int32)
    starts = first_pos + BLOCK * jnp.arange(rows // BLOCK, dtype=jnp.int32)
    positions = jnp.concatenate([offsets, starts]).astype(jnp.float32)
    table = pltpu.VMEM((rows, LANES), jnp.float32)
    return call(table_kernel, [positions[:, None] * inverse[None, :]], [table] * 2)


def rotate(acc, cosine, sine):
    half = HEAD_DIM // 2
    lane = lax.broadcasted_iota(jnp.int32, (acc.shape[0], LANES), 1)
    first = lane % HEAD_DIM < half
    partner = jnp.where(first, pltpu.roll(acc, LANES - half, 1), pltpu.roll(acc, half, 1))
    return acc * cosine + partner * sine


def half_rows(weight_ref, other):
    mine = lax.axis_index("tp")
    depth = weight_ref.shape[0] // 2
    half = 1 - mine if other else mine
    return pl.ds(pl.multiple_of(half * depth, depth), depth)


def key_value_own_kernel(
    tokens_ref, key_ref, value_ref, part_ref, own_ref, key_rest_ref, value_rest_ref, key_own_ref,
    value_own_ref, sems
):
    width = key_ref.shape[1]
    mine, rest = half_rows(key_ref, False), half_rows(key_ref, True)
    copies = [
        pltpu.make_async_copy(source, target, sems.at[i])
        for i, (source, target) in enumerate(
            [
                (tokens_ref, own_ref),
                (key_ref.at[mine, :], key_own_ref),
                (value_ref.at[mine, :], value_own_ref),
                (key_ref.at[rest, :], key_rest_ref),
                (value_ref.at[rest, :], value_rest_ref),
            ]
        )
    ]
    for copy in copies:
        copy.start()
    copies[0].wait()
    copies[1].wait()
    part_ref[:, :width] = dot(own_ref[...], key_own_ref[...])
    copies[2].wait()
    part_ref[:, width:] = dot(own_ref[...], value_own_ref[...])
    copies[3].wait()
    copies[4].wait()


def key_value_kernel(part_ref, other_ref, key_ref, value_ref, cos_ref, sin_ref, out_ref):
    width = key_ref.shape[1]
    key_acc = part_ref[:, :width] + dot(other_ref[...], key_ref[...])
    cosine, sine = cos_ref[...], sin_ref[...]
    for start in range(0, width, LANES):
        lanes = slice(start, start + LANES)
        out_ref[:, lanes] = rotate(key_acc[:, lanes], cosine, sine).astype(jnp.bfloat16)
    value_acc = part_ref[:, width:] + dot(other_ref[...], value_ref[...])
    out_ref[:, width:] = value_acc.astype(jnp.bfloat16)


def query_kernel(own_ref, other_ref, weight_ref, cos_ref, sin_ref, out_ref):
    acc = dot(own_ref[...], weight_ref[half_rows(weight_ref, False), :]) + dot(
        other_ref[...], weight_ref[half_rows(weight_ref, True), :]
    )
    cosine, sine = cos_ref[...], sin_ref[...]
    for start in range(0, acc.shape[1], LANES):
        lanes = slice(start, start + LANES)
        out_ref[:, lanes] = rotate(acc[:, lanes], cosine, sine).astype(jnp.bfloat16)


def pick_kernel(asked_ref, store_ref, out_ref):
    blocks = store_ref.shape[0] // BLOCK
    first = lax.axis_index("kv") * blocks
    asked = asked_ref[...]
    count = jnp.int32(0)
    index = [jnp.int32(0)] * CAP
    for block in range(blocks):
        hit = jnp.max((asked == first + block).astype(jnp.int32))
        for slot in range(CAP):
            index[slot] = jnp.where((hit == 1) & (count == slot), block, index[slot])
        count = count + hit
    for slot in range(CAP):
        rows = pl.ds(pl.multiple_of(index[slot] * BLOCK, BLOCK), BLOCK)
        out_ref[slot * BLOCK : (slot + 1) * BLOCK, :] = store_ref[rows, :]


def list_kernel(devices, chosen_ref, local_ref, remote_ref):
    blocks, slots = chosen_ref.shape
    rows = local_ref.shape[1]
    device = lax.axis_index("kv")
    spread = (
        lax.broadcasted_iota(jnp.int32, (blocks, rows), 1) // BLOCK
        == lax.broadcasted_iota(jnp.int32, (blocks, rows), 0)
    ).astype(jnp.float32)
    listed_ids = lax.dot_general(
        chosen_ref[...].astype(jnp.float32),
        spread,
        (((0,), (0,)), ((), ())),
        precision=lax.Precision.HIGHEST,
        preferred_element_type=jnp.float32,
    )
    row = lax.broadcasted_iota(jnp.int32, (blocks, rows), 0)
    for shift in range(devices):
        source = device - shift
        ids = jnp.where(source >= 0, source * blocks + row, -2).astype(jnp.float32)
        listed = jnp.zeros((blocks, rows), jnp.float32)
        for slot in range(slots):
            listed = jnp.where(listed_ids[slot : slot + 1, :] == ids, 1.0, listed)
        if shift == 0:
            local_ref[...] = jnp.where(listed > 0.0, 0.0, masked_score)
            continue
        needed = jnp.broadcast_to(jnp.max(listed, axis=1, keepdims=True), (blocks, rows))
        rank, step = needed, 1
        while step < blocks:
            rank = rank + jnp.where(row >= step, pltpu.roll(rank, step, 0), 0.0)
            step *= 2
        for slot in range(CAP):
            here = jnp.where((needed > 0.0) & (rank == slot + 1.0), listed, 0.0)
            hit = jnp.max(here, axis=0, keepdims=True)
            at = (shift - 1) * CAP + slot
            remote_ref[at : at + 1, :] = jnp.where(hit > 0.0, 0.0, masked_score)


def head_pair_queries(queries):
    lane = lax.broadcasted_iota(jnp.int32, queries.shape, 1)
    zero = jnp.zeros_like(queries)
    return jnp.concatenate(
        [jnp.where(lane < HEAD_DIM, queries, zero), jnp.where(lane < HEAD_DIM, zero, queries)],
        axis=0,
    )


def pair_scores(keys, queries):
    return lax.dot_general(
        keys, queries, (((1,), (1,)), ((), ())), preferred_element_type=jnp.float32
    )


def pair_values(values, weights):
    both = lax.dot_general(
        values, weights, (((0,), (0,)), ((), ())), preferred_element_type=jnp.float32
    )
    rows = weights.shape[1] // 2
    return jnp.concatenate([both[:HEAD_DIM, :rows], both[HEAD_DIM:, rows:]], axis=0)


def widen(stat):
    rows = stat.shape[1] // 2
    return jnp.concatenate(
        [
            jnp.broadcast_to(stat[:, :rows], (HEAD_DIM, rows)),
            jnp.broadcast_to(stat[:, rows:], (HEAD_DIM, rows)),
        ],
        axis=0,
    )


def local_kernel(query_ref, store_ref, bias_ref, peak_ref, total_ref, summed_ref):
    rows, width = query_ref.shape
    blocks = rows // BLOCK
    listed = jnp.concatenate(
        [jnp.broadcast_to(bias_ref[b : b + 1, :], (BLOCK, rows)) for b in range(blocks)], axis=0
    )
    key_row = lax.broadcasted_iota(jnp.int32, (rows, rows), 0)
    query_row = lax.broadcasted_iota(jnp.int32, (rows, rows), 1)
    bias = jnp.where(key_row <= query_row, listed, masked_score)
    bias = jnp.concatenate([bias, bias], axis=1)
    for pair in range(width // LANES):
        lanes = slice(pair * LANES, (pair + 1) * LANES)
        queries = head_pair_queries(query_ref[:, lanes])
        scores = pair_scores(store_ref[:, lanes], queries) + bias
        peak = jnp.max(scores, axis=0, keepdims=True)
        weights = jnp.exp2((scores - peak) * score_factor)
        peak_ref[pair : pair + 1, :] = peak
        total_ref[pair : pair + 1, :] = jnp.sum(weights, axis=0, keepdims=True)
        values = store_ref[:, width + pair * LANES : width + (pair + 1) * LANES]
        summed_ref[lanes, :] = pair_values(values, weights.astype(jnp.bfloat16))


def remote_kernel(shift, last, query_ref, bias_ref, got_ref, *refs):
    (peak_ref, total_ref, summed_ref), out_refs = refs[:3], refs[3:]
    rows, width = query_ref.shape
    first = (shift - 1) * CAP
    bias = jnp.concatenate(
        [jnp.broadcast_to(bias_ref[first + s : first + s + 1, :], (BLOCK, rows)) for s in range(CAP)],
        axis=0,
    )
    bias = jnp.concatenate([bias, bias], axis=1)
    for pair in range(width // LANES):
        lanes = slice(pair * LANES, (pair + 1) * LANES)
        queries = head_pair_queries(query_ref[:, lanes])
        peak = peak_ref[pair : pair + 1, :]
        scores = pair_scores(got_ref[:, lanes], queries) + bias
        peak_new = jnp.maximum(peak, jnp.max(scores, axis=0, keepdims=True))
        factor = jnp.exp2((peak - peak_new) * score_factor)
        weights = jnp.exp2((scores - peak_new) * score_factor)
        total = total_ref[pair : pair + 1, :] * factor + jnp.sum(weights, axis=0, keepdims=True)
        values = got_ref[:, width + pair * LANES : width + (pair + 1) * LANES]
        summed = summed_ref[lanes, :] * widen(factor) + pair_values(
            values, weights.astype(jnp.bfloat16)
        )
        if last:
            out_refs[0][:, lanes] = (summed / widen(total)).T.astype(jnp.bfloat16)
        else:
            out_refs[0][pair : pair + 1, :] = peak_new
            out_refs[1][pair : pair + 1, :] = total
            out_refs[2][lanes, :] = summed


def out_own_kernel(own_ref, weight_ref, out_ref):
    out_ref[...] = dot(own_ref[...], weight_ref[half_rows(weight_ref, False), :])


def out_kernel(part_ref, other_ref, weight_ref, out_ref, tile_ref, sems):
    tiles = tile_ref.shape[0]
    width = tile_ref.shape[2]
    rows = half_rows(weight_ref, True)
    copies = []
    for tile in range(tiles):
        lanes = slice(tile * width, (tile + 1) * width)
        acc = part_ref[:, lanes] + dot(other_ref[...], weight_ref[rows, lanes])
        tile_ref[tile] = acc.astype(jnp.bfloat16)
        copies.append(
            pltpu.make_async_copy(tile_ref.at[tile], out_ref.at[:, lanes], sems.at[tile])
        )
        copies[-1].start()
    for copy in copies:
        copy.wait()


def on_device(tokens, query_weight, key_weight, value_weight, out_weight, chosen):
    rows, depth = tokens.shape
    width = query_weight.shape[1]
    pairs = width // LANES
    device = lax.axis_index("kv")
    devices = lax.axis_size("kv")
    swap = [(0, 1), (1, 0)]

    def turn(x, by):
        return lax.ppermute(x, "kv", [(i, (i + by) % devices) for i in range(devices)])

    other = lax.ppermute(tokens, "tp", swap)
    asked = []
    for shift in range(1, devices):
        asked.append(turn(chosen, -shift))
    cosine, sine = rotary_tables(device * rows, rows)
    half = pltpu.VMEM((depth, width), jnp.bfloat16)
    part, own, key_rest, value_rest = call(
        key_value_own_kernel,
        [tokens, key_weight, value_weight],
        [
            pltpu.VMEM((rows, 2 * width), jnp.float32),
            pltpu.VMEM((rows, depth), jnp.bfloat16),
            half,
            half,
        ],
        flops=4 * rows * depth * width,
        scratch=[half, half, pltpu.SemaphoreType.DMA((5,))],
        far=3,
    )
    store = call(
        key_value_kernel,
        [part, other, key_rest, value_rest, cosine, sine],
        [pltpu.VMEM((rows, 2 * width), jnp.bfloat16)],
        flops=4 * rows * depth * width,
    )
    got = []
    for shift in range(1, devices):
        picked = call(
            pick_kernel,
            [asked[shift - 1], store],
            [pltpu.VMEM((CAP * BLOCK, 2 * width), jnp.bfloat16)],
        )
        got.append(turn(picked, shift))
    queries = call(
        query_kernel,
        [own, other, query_weight, cosine, sine],
        [pltpu.VMEM((rows, width), jnp.bfloat16)],
        flops=4 * rows * depth * width,
    )
    remote_rows = max(8, (devices - 1) * CAP)
    local_bias, remote_bias = call(
        functools.partial(list_kernel, devices),
        [chosen],
        [
            pltpu.VMEM((rows // BLOCK, rows), jnp.float32),
            pltpu.VMEM((remote_rows, rows), jnp.float32),
        ],
    )
    state_shapes = [
        pltpu.VMEM((pairs, 2 * rows), jnp.float32),
        pltpu.VMEM((pairs, 2 * rows), jnp.float32),
        pltpu.VMEM((width, rows), jnp.float32),
    ]
    attended_shape = [pltpu.VMEM((rows, width), jnp.bfloat16)]
    state = call(
        local_kernel, [queries, store, local_bias], state_shapes, flops=16 * rows * rows * width
    )
    for shift in range(1, devices):
        last = shift == devices - 1
        state = call(
            functools.partial(remote_kernel, shift, last),
            [queries, remote_bias, got[shift - 1], *state],
            attended_shape if last else state_shapes,
            flops=16 * rows * CAP * BLOCK * width,
        )
    attended = state
    attended_other = lax.ppermute(attended, "tp", swap)
    out_width = out_weight.shape[1]
    out_part = call(
        out_own_kernel,
        [attended, out_weight],
        [pltpu.VMEM((rows, out_width), jnp.float32)],
        flops=2 * rows * width * out_width,
    )
    tiles = 4
    return call(
        out_kernel,
        [out_part, attended_other, out_weight],
        [pltpu.HBM((rows, out_width), jnp.bfloat16)],
        flops=2 * rows * width * out_width,
        scratch=[
            pltpu.VMEM((tiles, rows, out_width // tiles), jnp.bfloat16),
            pltpu.SemaphoreType.DMA((tiles,)),
        ],
    )


def solution(mesh):
    placed = (
        P(("dp", "kv"), "tp"),
        P(None, "tp"),
        P(None, "tp"),
        P(None, "tp"),
        P(None, "tp"),
        P(("dp", "kv"), None),
    )
    return jax.shard_map(
        on_device, mesh=mesh, in_specs=placed, out_specs=P(("dp", "kv"), "tp"), check_vma=False
    )
```

```python
import functools

import jax
import jax.numpy as jnp
from jax import lax
from jax.experimental import pallas as pl
from jax.experimental.pallas import tpu as pltpu
from jax.sharding import PartitionSpec as P


HEAD_DIM = 64
BLOCK = 32
CAP = 3
LANES = 128

rotary_base = 500000.0
masked_score = -1e30
score_factor = HEAD_DIM ** (-0.5) * 1.4426950408889634


VMEM = pl.BlockSpec(memory_space=pltpu.VMEM)


def source_of(device, turn, devices):
    if devices & (devices - 1) == 0:
        return device ^ turn
    return (device + devices - turn) % devices


def turn_order(devices):
    return [*range(2, devices), 1] if devices > 1 else []


def call(kernel, operands, results, flops=1000000, limit=16, scratch=(), far=0):
    anywhere = pl.BlockSpec(memory_space=pl.ANY)
    near = len(operands) - far
    out = pl.pallas_call(
        kernel,
        in_specs=[VMEM] * near + [anywhere] * far,
        out_specs=[anywhere if r.memory_space == pltpu.HBM else VMEM for r in results],
        out_shape=results,
        scratch_shapes=list(scratch),
        cost_estimate=pl.CostEstimate(flops=flops, bytes_accessed=100000, transcendentals=0),
        compiler_params=pltpu.CompilerParams(vmem_limit_bytes=limit << 20),
    )(
        *[pltpu.with_memory_space_constraint(x, pltpu.VMEM) for x in operands[:near]],
        *[pltpu.with_memory_space_constraint(x, pltpu.HBM) for x in operands[near:]],
    )
    return out[0] if len(results) == 1 else out


def dot(left, right):
    return jnp.dot(left, right, preferred_element_type=jnp.float32)


def table_kernel(cos_ref, sin_ref):
    rows = cos_ref.shape[0]
    half = HEAD_DIM // 2
    lane = lax.broadcasted_iota(jnp.int32, (BLOCK, LANES), 1) % half
    inverse = jnp.zeros((BLOCK, LANES), jnp.float32)
    for j in range(half):
        inverse = jnp.where(lane == j, float(1.0 / rotary_base ** (j / half)), inverse)
    offset = lax.broadcasted_iota(jnp.int32, (BLOCK, LANES), 0)
    start = lax.axis_index("kv") * rows + BLOCK * offset
    sign = jnp.where(
        lax.broadcasted_iota(jnp.int32, (BLOCK, LANES), 1) % HEAD_DIM < half, -1.0, 1.0
    )
    angle_in = offset.astype(jnp.float32) * inverse
    cos_in, sin_in = jnp.cos(angle_in), jnp.sin(angle_in)
    angle_at = start.astype(jnp.float32) * inverse
    cos_at, sin_at = jnp.cos(angle_at), jnp.sin(angle_at)
    for block in range(rows // BLOCK):
        at = slice(block * BLOCK, (block + 1) * BLOCK)
        cos_b, sin_b = cos_at[block : block + 1], sin_at[block : block + 1]
        cos_ref[at, :] = cos_in * cos_b - sin_in * sin_b
        sin_ref[at, :] = (sin_in * cos_b + cos_in * sin_b) * sign


def rotary_tables(rows):
    table = pltpu.VMEM((rows, LANES), jnp.float32)
    return call(table_kernel, [], [table] * 2, flops=2000000000)


def rotate(acc, cosine, sine):
    half = HEAD_DIM // 2
    lane = lax.broadcasted_iota(jnp.int32, (acc.shape[0], LANES), 1)
    first = lane % HEAD_DIM < half
    partner = jnp.where(first, pltpu.roll(acc, LANES - half, 1), pltpu.roll(acc, half, 1))
    return acc * cosine + partner * sine


def half_rows(weight_ref, other):
    mine = lax.axis_index("tp")
    depth = weight_ref.shape[0] // 2
    half = 1 - mine if other else mine
    return pl.ds(pl.multiple_of(half * depth, depth), depth)


def key_value_own_kernel(own_ref, key_ref, value_ref, out_ref):
    width = key_ref.shape[1]
    rows = half_rows(key_ref, False)
    out_ref[:, :width] = dot(own_ref[...], key_ref[rows, :])
    out_ref[:, width:] = dot(own_ref[...], value_ref[rows, :])


def key_value_kernel(part_ref, other_ref, key_ref, value_ref, cos_ref, sin_ref, out_ref):
    width = key_ref.shape[1]
    rows = half_rows(key_ref, True)
    key_acc = part_ref[:, :width] + dot(other_ref[...], key_ref[rows, :])
    cosine, sine = cos_ref[...], sin_ref[...]
    for start in range(0, width, LANES):
        lanes = slice(start, start + LANES)
        out_ref[:, lanes] = rotate(key_acc[:, lanes], cosine, sine).astype(jnp.bfloat16)
    value_acc = part_ref[:, width:] + dot(other_ref[...], value_ref[rows, :])
    out_ref[:, width:] = value_acc.astype(jnp.bfloat16)


def query_kernel(own_ref, other_ref, weight_ref, cos_ref, sin_ref, out_ref):
    acc = dot(own_ref[...], weight_ref[half_rows(weight_ref, False), :]) + dot(
        other_ref[...], weight_ref[half_rows(weight_ref, True), :]
    )
    cosine, sine = cos_ref[...], sin_ref[...]
    for start in range(0, acc.shape[1], LANES):
        lanes = slice(start, start + LANES)
        out_ref[:, lanes] = rotate(acc[:, lanes], cosine, sine).astype(jnp.bfloat16)


def pick_kernel(asked_ref, store_ref, out_ref):
    blocks = store_ref.shape[0] // BLOCK
    first = lax.axis_index("kv") * blocks
    asked = asked_ref[...]
    count = jnp.int32(0)
    index = [jnp.int32(0)] * CAP
    for block in range(blocks):
        hit = jnp.max((asked == first + block).astype(jnp.int32))
        for slot in range(CAP):
            index[slot] = jnp.where((hit == 1) & (count == slot), block, index[slot])
        count = count + hit
    for slot in range(CAP):
        rows = pl.ds(pl.multiple_of(index[slot] * BLOCK, BLOCK), BLOCK)
        out_ref[slot * BLOCK : (slot + 1) * BLOCK, :] = store_ref[rows, :]


def list_kernel(devices, turns, far_ref, local_ref, remote_ref, chosen_ref, sem):
    copy = pltpu.make_async_copy(far_ref, chosen_ref, sem)
    copy.start()
    copy.wait()
    blocks, slots = chosen_ref.shape
    rows = local_ref.shape[1]
    device = lax.axis_index("kv")
    spread = (
        lax.broadcasted_iota(jnp.int32, (blocks, rows), 1) // BLOCK
        == lax.broadcasted_iota(jnp.int32, (blocks, rows), 0)
    ).astype(jnp.float32)
    listed_ids = lax.dot_general(
        chosen_ref[...].astype(jnp.float32),
        spread,
        (((0,), (0,)), ((), ())),
        precision=lax.Precision.HIGHEST,
        preferred_element_type=jnp.float32,
    )
    row = lax.broadcasted_iota(jnp.int32, (blocks, rows), 0)
    for place, turn in enumerate([0, *turns]):
        source = source_of(device, turn, devices)
        ids = jnp.where(source <= device, source * blocks + row, -2).astype(jnp.float32)
        listed = jnp.zeros((blocks, rows), jnp.float32)
        for slot in range(slots):
            listed = jnp.where(listed_ids[slot : slot + 1, :] == ids, 1.0, listed)
        if turn == 0:
            local_ref[...] = jnp.where(listed > 0.0, 0.0, masked_score)
            continue
        needed = jnp.broadcast_to(jnp.max(listed, axis=1, keepdims=True), (blocks, rows))
        rank, step = needed, 1
        while step < blocks:
            rank = rank + jnp.where(row >= step, pltpu.roll(rank, step, 0), 0.0)
            step *= 2
        for slot in range(CAP):
            here = jnp.where((needed > 0.0) & (rank == slot + 1.0), listed, 0.0)
            hit = jnp.max(here, axis=0, keepdims=True)
            at = (place - 1) * CAP + slot
            remote_ref[at : at + 1, :] = jnp.where(hit > 0.0, 0.0, masked_score)


def head_pair_queries(queries):
    lane = lax.broadcasted_iota(jnp.int32, queries.shape, 1)
    zero = jnp.zeros_like(queries)
    return jnp.concatenate(
        [jnp.where(lane < HEAD_DIM, queries, zero), jnp.where(lane < HEAD_DIM, zero, queries)],
        axis=0,
    )


def pair_scores(keys, queries):
    return lax.dot_general(
        keys, queries, (((1,), (1,)), ((), ())), preferred_element_type=jnp.float32
    )


def pair_values(values, weights):
    both = lax.dot_general(
        values, weights, (((0,), (0,)), ((), ())), preferred_element_type=jnp.float32
    )
    rows = weights.shape[1] // 2
    return jnp.concatenate([both[:HEAD_DIM, :rows], both[HEAD_DIM:, rows:]], axis=0)


def widen(stat):
    rows = stat.shape[1] // 2
    return jnp.concatenate(
        [
            jnp.broadcast_to(stat[:, :rows], (HEAD_DIM, rows)),
            jnp.broadcast_to(stat[:, rows:], (HEAD_DIM, rows)),
        ],
        axis=0,
    )


def local_kernel(query_ref, store_ref, bias_ref, peak_ref, total_ref, summed_ref):
    rows, width = query_ref.shape
    blocks = rows // BLOCK
    listed = jnp.concatenate(
        [jnp.broadcast_to(bias_ref[b : b + 1, :], (BLOCK, rows)) for b in range(blocks)], axis=0
    )
    key_row = lax.broadcasted_iota(jnp.int32, (rows, rows), 0)
    query_row = lax.broadcasted_iota(jnp.int32, (rows, rows), 1)
    bias = jnp.where(key_row <= query_row, listed, masked_score)
    bias = jnp.concatenate([bias, bias], axis=1)
    for pair in range(width // LANES):
        lanes = slice(pair * LANES, (pair + 1) * LANES)
        queries = head_pair_queries(query_ref[:, lanes])
        scores = pair_scores(store_ref[:, lanes], queries) + bias
        peak = jnp.max(scores, axis=0, keepdims=True)
        weights = jnp.exp2((scores - peak) * score_factor)
        peak_ref[pair : pair + 1, :] = peak
        total_ref[pair : pair + 1, :] = jnp.sum(weights, axis=0, keepdims=True)
        values = store_ref[:, width + pair * LANES : width + (pair + 1) * LANES]
        summed_ref[lanes, :] = pair_values(values, weights.astype(jnp.bfloat16))


def remote_kernel(first, parts, last, query_ref, bias_ref, *refs):
    got_refs, (peak_ref, total_ref, summed_ref) = refs[:parts], refs[parts : parts + 3]
    out_refs = refs[parts + 3 :]
    rows, width = query_ref.shape
    pairs = [slice(p * LANES, (p + 1) * LANES) for p in range(width // LANES)]
    spans = [slice(width + p.start, width + p.stop) for p in pairs]
    slots = range(first * CAP, (first + parts) * CAP)
    bias = jnp.concatenate(
        [jnp.broadcast_to(bias_ref[s : s + 1, :], (BLOCK, rows)) for s in slots], axis=0
    )
    bias = jnp.concatenate([bias, bias], axis=1)
    scores = []
    for lanes in pairs:
        keys = jnp.concatenate([got[:, lanes] for got in got_refs], axis=0)
        scores.append(pair_scores(keys, head_pair_queries(query_ref[:, lanes])) + bias)
    weights, factors, totals = [], [], []
    for pair in range(len(pairs)):
        peak = peak_ref[pair : pair + 1, :]
        peak_new = jnp.maximum(peak, jnp.max(scores[pair], axis=0, keepdims=True))
        factor = jnp.exp2((peak - peak_new) * score_factor)
        weight = jnp.exp2((scores[pair] - peak_new) * score_factor)
        total = total_ref[pair : pair + 1, :] * factor + jnp.sum(weight, axis=0, keepdims=True)
        weights.append(weight.astype(jnp.bfloat16))
        factors.append(factor)
        totals.append(total)
        if not last:
            out_refs[0][pair : pair + 1, :] = peak_new
            out_refs[1][pair : pair + 1, :] = total
    added = []
    for pair, lanes in enumerate(spans):
        values = jnp.concatenate([got[:, lanes] for got in got_refs], axis=0)
        added.append(pair_values(values, weights[pair]))
    for pair, lanes in enumerate(pairs):
        if last:
            over = 1.0 / totals[pair]
            summed = summed_ref[lanes, :] * widen(factors[pair] * over) + added[pair] * widen(over)
            out_refs[0][:, lanes] = summed.T.astype(jnp.bfloat16)
        else:
            out_refs[2][lanes, :] = summed_ref[lanes, :] * widen(factors[pair]) + added[pair]


def out_own_kernel(own_ref, weight_ref, out_ref):
    out_ref[...] = dot(own_ref[...], weight_ref[half_rows(weight_ref, False), :])


def out_kernel(part_ref, other_ref, weight_ref, out_ref, tile_ref, sems):
    tiles = tile_ref.shape[0]
    width = tile_ref.shape[2]
    rows = half_rows(weight_ref, True)
    copies = []
    for tile in range(tiles):
        lanes = slice(tile * width, (tile + 1) * width)
        acc = part_ref[:, lanes] + dot(other_ref[...], weight_ref[rows, lanes])
        tile_ref[tile] = acc.astype(jnp.bfloat16)
        copies.append(
            pltpu.make_async_copy(tile_ref.at[tile], out_ref.at[:, lanes], sems.at[tile])
        )
        copies[-1].start()
    for copy in copies:
        copy.wait()


def on_device(tokens, query_weight, key_weight, value_weight, out_weight, chosen):
    rows, depth = tokens.shape
    width = query_weight.shape[1]
    pairs = width // LANES
    devices = lax.axis_size("kv")
    swap = [(0, 1), (1, 0)]

    def ask(x, turn):
        return lax.ppermute(x, "kv", [(i, source_of(i, turn, devices)) for i in range(devices)])

    def send(x, turn):
        return lax.ppermute(x, "kv", [(source_of(i, turn, devices), i) for i in range(devices)])

    other = lax.ppermute(tokens, "tp", swap)
    asked, turns = [], turn_order(devices)
    for shift in turns:
        asked.append(ask(chosen, shift))
    cosine, sine = rotary_tables(rows)
    part = call(
        key_value_own_kernel,
        [tokens, key_weight, value_weight],
        [pltpu.VMEM((rows, 2 * width), jnp.float32)],
        flops=4 * rows * depth * width,
    )
    store = call(
        key_value_kernel,
        [part, other, key_weight, value_weight, cosine, sine],
        [pltpu.VMEM((rows, 2 * width), jnp.bfloat16)],
        flops=4 * rows * depth * width,
    )
    got = []
    for shift, asked_by in zip(turns, asked):
        picked = call(
            pick_kernel, [asked_by, store], [pltpu.VMEM((CAP * BLOCK, 2 * width), jnp.bfloat16)]
        )
        got.append(send(picked, shift))
    queries = call(
        query_kernel,
        [tokens, other, query_weight, cosine, sine],
        [pltpu.VMEM((rows, width), jnp.bfloat16)],
        flops=4 * rows * depth * width,
    )
    remote_rows = max(8, (devices - 1) * CAP)
    local_bias, remote_bias = call(
        functools.partial(list_kernel, devices, turns),
        [chosen],
        [
            pltpu.VMEM((rows // BLOCK, rows), jnp.float32),
            pltpu.VMEM((remote_rows, rows), jnp.float32),
        ],
        scratch=[pltpu.VMEM(chosen.shape, chosen.dtype), pltpu.SemaphoreType.DMA],
        far=1,
    )
    state_shapes = [
        pltpu.VMEM((pairs, 2 * rows), jnp.float32),
        pltpu.VMEM((pairs, 2 * rows), jnp.float32),
        pltpu.VMEM((width, rows), jnp.float32),
    ]
    attended_shape = [pltpu.VMEM((rows, width), jnp.bfloat16)]
    state = call(
        local_kernel, [queries, store, local_bias], state_shapes, flops=16 * rows * rows * width
    )
    final = max(0, len(got) - 2)
    groups = [(i, 1) for i in range(final)] + [(final, len(got) - final)]
    for first, parts in groups:
        last = first + parts == len(got)
        if parts == 0:
            continue
        state = call(
            functools.partial(remote_kernel, first, parts, last),
            [queries, remote_bias, *got[first : first + parts], *state],
            attended_shape if last else state_shapes,
            flops=16 * rows * parts * CAP * BLOCK * width,
        )
    attended = state
    attended_other = lax.ppermute(attended, "tp", swap)
    out_width = out_weight.shape[1]
    out_part = call(
        out_own_kernel,
        [attended, out_weight],
        [pltpu.VMEM((rows, out_width), jnp.float32)],
        flops=2 * rows * width * out_width,
    )
    tiles = 4
    return call(
        out_kernel,
        [out_part, attended_other, out_weight],
        [pltpu.HBM((rows, out_width), jnp.bfloat16)],
        flops=2 * rows * width * out_width,
        scratch=[
            pltpu.VMEM((tiles, rows, out_width // tiles), jnp.bfloat16),
            pltpu.SemaphoreType.DMA((tiles,)),
        ],
    )


def solution(mesh):
    placed = (
        P(("dp", "kv"), "tp"),
        P(None, "tp"),
        P(None, "tp"),
        P(None, "tp"),
        P(None, "tp"),
        P(("dp", "kv"), None),
    )
    return jax.shard_map(
        on_device, mesh=mesh, in_specs=placed, out_specs=P(("dp", "kv"), "tp"), check_vma=False
    )
```

```python
import functools

import jax
import jax.numpy as jnp
from jax import lax
from jax.experimental import pallas as pl
from jax.experimental.pallas import tpu as pltpu
from jax.sharding import PartitionSpec as P


HEAD_DIM = 64
BLOCK = 32
CAP = 3
LANES = 128

rotary_base = 500000.0
masked_score = -1e30
score_factor = HEAD_DIM ** (-0.5) * 1.4426950408889634


VMEM = pl.BlockSpec(memory_space=pltpu.VMEM)


def source_of(device, turn, devices):
    if devices & (devices - 1) == 0:
        return device ^ turn
    return (device + devices - turn) % devices


def turn_order(devices):
    last = devices - 1
    return [*range(2, last), *([1] if last > 1 else []), last]


def call(kernel, operands, results, flops=1000000, limit=16, scratch=(), far=0):
    anywhere = pl.BlockSpec(memory_space=pl.ANY)
    near = len(operands) - far
    out = pl.pallas_call(
        kernel,
        in_specs=[VMEM] * near + [anywhere] * far,
        out_specs=[anywhere if r.memory_space == pltpu.HBM else VMEM for r in results],
        out_shape=results,
        scratch_shapes=list(scratch),
        cost_estimate=pl.CostEstimate(flops=flops, bytes_accessed=100000, transcendentals=0),
        compiler_params=pltpu.CompilerParams(vmem_limit_bytes=limit << 20),
    )(
        *[pltpu.with_memory_space_constraint(x, pltpu.VMEM) for x in operands[:near]],
        *[pltpu.with_memory_space_constraint(x, pltpu.HBM) for x in operands[near:]],
    )
    return out[0] if len(results) == 1 else out


def dot(left, right):
    return jnp.dot(left, right, preferred_element_type=jnp.float32)


def table_kernel(cos_ref, sin_ref):
    rows = cos_ref.shape[0]
    half = HEAD_DIM // 2
    lane = lax.broadcasted_iota(jnp.int32, (BLOCK, LANES), 1) % half
    inverse = jnp.zeros((BLOCK, LANES), jnp.float32)
    for j in range(half):
        inverse = jnp.where(lane == j, float(1.0 / rotary_base ** (j / half)), inverse)
    offset = lax.broadcasted_iota(jnp.int32, (BLOCK, LANES), 0)
    start = lax.axis_index("kv") * rows + BLOCK * offset
    sign = jnp.where(
        lax.broadcasted_iota(jnp.int32, (BLOCK, LANES), 1) % HEAD_DIM < half, -1.0, 1.0
    )
    angle_in = offset.astype(jnp.float32) * inverse
    cos_in, sin_in = jnp.cos(angle_in), jnp.sin(angle_in)
    angle_at = start.astype(jnp.float32) * inverse
    cos_at, sin_at = jnp.cos(angle_at), jnp.sin(angle_at)
    for block in range(rows // BLOCK):
        at = slice(block * BLOCK, (block + 1) * BLOCK)
        cos_b, sin_b = cos_at[block : block + 1], sin_at[block : block + 1]
        cos_ref[at, :] = cos_in * cos_b - sin_in * sin_b
        sin_ref[at, :] = (sin_in * cos_b + cos_in * sin_b) * sign


def rotary_tables(rows):
    table = pltpu.VMEM((rows, LANES), jnp.float32)
    return call(table_kernel, [], [table] * 2, flops=2000000000)


def rotate(acc, cosine, sine):
    half = HEAD_DIM // 2
    lane = lax.broadcasted_iota(jnp.int32, (acc.shape[0], LANES), 1)
    first = lane % HEAD_DIM < half
    partner = jnp.where(first, pltpu.roll(acc, LANES - half, 1), pltpu.roll(acc, half, 1))
    return acc * cosine + partner * sine


def half_rows(weight_ref, other):
    mine = lax.axis_index("tp")
    depth = weight_ref.shape[0] // 2
    half = 1 - mine if other else mine
    return pl.ds(pl.multiple_of(half * depth, depth), depth)


def key_value_own_kernel(own_ref, key_ref, value_ref, out_ref):
    width = key_ref.shape[1]
    rows = half_rows(key_ref, False)
    out_ref[:, :width] = dot(own_ref[...], key_ref[rows, :])
    out_ref[:, width:] = dot(own_ref[...], value_ref[rows, :])


def key_value_kernel(part_ref, other_ref, key_ref, value_ref, cos_ref, sin_ref, out_ref):
    width = key_ref.shape[1]
    rows = half_rows(key_ref, True)
    key_acc = part_ref[:, :width] + dot(other_ref[...], key_ref[rows, :])
    cosine, sine = cos_ref[...], sin_ref[...]
    for start in range(0, width, LANES):
        lanes = slice(start, start + LANES)
        out_ref[:, lanes] = rotate(key_acc[:, lanes], cosine, sine).astype(jnp.bfloat16)
    value_acc = part_ref[:, width:] + dot(other_ref[...], value_ref[rows, :])
    out_ref[:, width:] = value_acc.astype(jnp.bfloat16)


def query_kernel(own_ref, other_ref, weight_ref, cos_ref, sin_ref, out_ref):
    acc = dot(own_ref[...], weight_ref[half_rows(weight_ref, False), :]) + dot(
        other_ref[...], weight_ref[half_rows(weight_ref, True), :]
    )
    cosine, sine = cos_ref[...], sin_ref[...]
    for start in range(0, acc.shape[1], LANES):
        lanes = slice(start, start + LANES)
        out_ref[:, lanes] = rotate(acc[:, lanes], cosine, sine).astype(jnp.bfloat16)


def pick_kernel(cuts, asked_ref, store_ref, *out_refs):
    blocks = store_ref.shape[0] // BLOCK
    width = store_ref.shape[1] // 2
    first = lax.axis_index("kv") * blocks
    asked = asked_ref[...]
    count = jnp.int32(0)
    index = [jnp.int32(0)] * CAP
    for block in range(blocks):
        hit = jnp.max((asked == first + block).astype(jnp.int32))
        for slot in range(CAP):
            index[slot] = jnp.where((hit == 1) & (count == slot), block, index[slot])
        count = count + hit
    for (low, high), out_ref in zip(cuts, out_refs):
        for slot in range(CAP):
            rows = pl.ds(pl.multiple_of(index[slot] * BLOCK, BLOCK), BLOCK)
            place = slice(slot * BLOCK, (slot + 1) * BLOCK)
            out_ref[place, : high - low] = store_ref[rows, low:high]
            out_ref[place, high - low :] = store_ref[rows, width + low : width + high]


def list_kernel(devices, turns, far_ref, local_ref, remote_ref, chosen_ref, sem):
    copy = pltpu.make_async_copy(far_ref, chosen_ref, sem)
    copy.start()
    copy.wait()
    blocks, slots = chosen_ref.shape
    rows = local_ref.shape[1]
    device = lax.axis_index("kv")
    spread = (
        lax.broadcasted_iota(jnp.int32, (blocks, rows), 1) // BLOCK
        == lax.broadcasted_iota(jnp.int32, (blocks, rows), 0)
    ).astype(jnp.float32)
    listed_ids = lax.dot_general(
        chosen_ref[...].astype(jnp.float32),
        spread,
        (((0,), (0,)), ((), ())),
        precision=lax.Precision.HIGHEST,
        preferred_element_type=jnp.float32,
    )
    row = lax.broadcasted_iota(jnp.int32, (blocks, rows), 0)
    for place, turn in enumerate([0, *turns]):
        source = source_of(device, turn, devices)
        ids = jnp.where(source <= device, source * blocks + row, -2).astype(jnp.float32)
        listed = jnp.zeros((blocks, rows), jnp.float32)
        for slot in range(slots):
            listed = jnp.where(listed_ids[slot : slot + 1, :] == ids, 1.0, listed)
        if turn == 0:
            local_ref[...] = jnp.where(listed > 0.0, 0.0, masked_score)
            continue
        needed = jnp.broadcast_to(jnp.max(listed, axis=1, keepdims=True), (blocks, rows))
        rank, step = needed, 1
        while step < blocks:
            rank = rank + jnp.where(row >= step, pltpu.roll(rank, step, 0), 0.0)
            step *= 2
        for slot in range(CAP):
            here = jnp.where((needed > 0.0) & (rank == slot + 1.0), listed, 0.0)
            hit = jnp.max(here, axis=0, keepdims=True)
            at = (place - 1) * CAP + slot
            remote_ref[at : at + 1, :] = jnp.where(hit > 0.0, 0.0, masked_score)


def head_pair_queries(queries):
    lane = lax.broadcasted_iota(jnp.int32, queries.shape, 1)
    zero = jnp.zeros_like(queries)
    return jnp.concatenate(
        [jnp.where(lane < HEAD_DIM, queries, zero), jnp.where(lane < HEAD_DIM, zero, queries)],
        axis=0,
    )


def pair_scores(keys, queries):
    return lax.dot_general(
        keys, queries, (((1,), (1,)), ((), ())), preferred_element_type=jnp.float32
    )


def pair_values(values, weights):
    both = lax.dot_general(
        values, weights, (((0,), (0,)), ((), ())), preferred_element_type=jnp.float32
    )
    rows = weights.shape[1] // 2
    return jnp.concatenate([both[:HEAD_DIM, :rows], both[HEAD_DIM:, rows:]], axis=0)


def widen(stat):
    rows = stat.shape[1] // 2
    return jnp.concatenate(
        [
            jnp.broadcast_to(stat[:, :rows], (HEAD_DIM, rows)),
            jnp.broadcast_to(stat[:, rows:], (HEAD_DIM, rows)),
        ],
        axis=0,
    )


def local_kernel(query_ref, store_ref, bias_ref, peak_ref, total_ref, summed_ref):
    rows, width = query_ref.shape
    blocks = rows // BLOCK
    listed = jnp.concatenate(
        [jnp.broadcast_to(bias_ref[b : b + 1, :], (BLOCK, rows)) for b in range(blocks)], axis=0
    )
    key_row = lax.broadcasted_iota(jnp.int32, (rows, rows), 0)
    query_row = lax.broadcasted_iota(jnp.int32, (rows, rows), 1)
    bias = jnp.where(key_row <= query_row, listed, masked_score)
    bias = jnp.concatenate([bias, bias], axis=1)
    for pair in range(width // LANES):
        lanes = slice(pair * LANES, (pair + 1) * LANES)
        queries = head_pair_queries(query_ref[:, lanes])
        scores = pair_scores(store_ref[:, lanes], queries) + bias
        peak = jnp.max(scores, axis=0, keepdims=True)
        weights = jnp.exp2((scores - peak) * score_factor)
        peak_ref[pair : pair + 1, :] = peak
        total_ref[pair : pair + 1, :] = jnp.sum(weights, axis=0, keepdims=True)
        values = store_ref[:, width + pair * LANES : width + (pair + 1) * LANES]
        summed_ref[lanes, :] = pair_values(values, weights.astype(jnp.bfloat16))


def remote_kernel(place, low, last, query_ref, bias_ref, got_ref, *refs):
    (peak_ref, total_ref, summed_ref), out_refs = refs[:3], refs[3:]
    rows = query_ref.shape[0]
    width = got_ref.shape[1] // 2
    count = width // LANES
    bias = jnp.concatenate(
        [
            jnp.broadcast_to(bias_ref[s : s + 1, :], (BLOCK, rows))
            for s in range(place * CAP, (place + 1) * CAP)
        ],
        axis=0,
    )
    bias = jnp.concatenate([bias, bias], axis=1)
    here = [slice(p * LANES, (p + 1) * LANES) for p in range(count)]
    lanes = [slice(low + h.start, low + h.stop) for h in here]
    stats = [low // LANES + p for p in range(count)]
    scores = [
        pair_scores(got_ref[:, here[p]], head_pair_queries(query_ref[:, lanes[p]])) + bias
        for p in range(count)
    ]
    weights, factors, totals = [], [], []
    for p, at in enumerate(stats):
        peak = peak_ref[at : at + 1, :]
        peak_new = jnp.maximum(peak, jnp.max(scores[p], axis=0, keepdims=True))
        factor = jnp.exp2((peak - peak_new) * score_factor)
        weight = jnp.exp2((scores[p] - peak_new) * score_factor)
        total = total_ref[at : at + 1, :] * factor + jnp.sum(weight, axis=0, keepdims=True)
        weights.append(weight.astype(jnp.bfloat16))
        factors.append(factor)
        totals.append(total)
        if not last:
            out_refs[0][at : at + 1, :] = peak_new
            out_refs[1][at : at + 1, :] = total
    added = [
        pair_values(got_ref[:, width + here[p].start : width + here[p].stop], weights[p])
        for p in range(count)
    ]
    for p in range(count):
        if last:
            over = 1.0 / totals[p]
            summed = summed_ref[lanes[p], :] * widen(factors[p] * over) + added[p] * widen(over)
            out_refs[0][:, here[p]] = summed.T.astype(jnp.bfloat16)
        else:
            out_refs[2][lanes[p], :] = summed_ref[lanes[p], :] * widen(factors[p]) + added[p]


def head_rows(weight_ref, other, low, width):
    mine = lax.axis_index("tp")
    depth = weight_ref.shape[0] // 2
    half = 1 - mine if other else mine
    return pl.ds(pl.multiple_of(half * depth + low, LANES), width)


def out_first_kernel(own_ref, other_ref, weight_ref, out_ref):
    width = own_ref.shape[1]
    out_ref[...] = dot(own_ref[...], weight_ref[head_rows(weight_ref, False, 0, width), :]) + dot(
        other_ref[...], weight_ref[head_rows(weight_ref, True, 0, width), :]
    )


def out_own_kernel(low, part_ref, own_ref, weight_ref, out_ref):
    rows = head_rows(weight_ref, False, low, own_ref.shape[1])
    out_ref[...] = part_ref[...] + dot(own_ref[...], weight_ref[rows, :])


def out_kernel(low, part_ref, other_ref, weight_ref, out_ref, tile_ref, sems):
    tiles = tile_ref.shape[0]
    width = tile_ref.shape[2]
    rows = head_rows(weight_ref, True, low, other_ref.shape[1])
    copies = []
    for tile in range(tiles):
        lanes = slice(tile * width, (tile + 1) * width)
        acc = part_ref[:, lanes] + dot(other_ref[...], weight_ref[rows, lanes])
        tile_ref[tile] = acc.astype(jnp.bfloat16)
        copies.append(
            pltpu.make_async_copy(tile_ref.at[tile], out_ref.at[:, lanes], sems.at[tile])
        )
        copies[-1].start()
    for copy in copies:
        copy.wait()


def on_device(tokens, query_weight, key_weight, value_weight, out_weight, chosen):
    rows, depth = tokens.shape
    width = query_weight.shape[1]
    pairs = width // LANES
    devices = lax.axis_size("kv")
    swap = [(0, 1), (1, 0)]

    def ask(x, turn):
        return lax.ppermute(x, "kv", [(i, source_of(i, turn, devices)) for i in range(devices)])

    def send(x, turn):
        return lax.ppermute(x, "kv", [(source_of(i, turn, devices), i) for i in range(devices)])

    other = lax.ppermute(tokens, "tp", swap)
    asked, turns = [], turn_order(devices)
    for turn in turns:
        asked.append(ask(chosen, turn))
    cosine, sine = rotary_tables(rows)
    part = call(
        key_value_own_kernel,
        [tokens, key_weight, value_weight],
        [pltpu.VMEM((rows, 2 * width), jnp.float32)],
        flops=4 * rows * depth * width,
    )
    store = call(
        key_value_kernel,
        [part, other, key_weight, value_weight, cosine, sine],
        [pltpu.VMEM((rows, 2 * width), jnp.bfloat16)],
        flops=4 * rows * depth * width,
    )
    cut = width // 2
    cuts = [(0, cut), (cut, width)]
    got = []
    for turn, asked_by in zip(turns, asked):
        parts = cuts if turn == turns[-1] else [(0, width)]
        picked = call(
            functools.partial(pick_kernel, parts),
            [asked_by, store],
            [pltpu.VMEM((CAP * BLOCK, 2 * (high - low)), jnp.bfloat16) for low, high in parts],
        )
        for part, block in enumerate(picked if len(parts) > 1 else [picked]):
            got.append(send(block, turn))
    queries = call(
        query_kernel,
        [tokens, other, query_weight, cosine, sine],
        [pltpu.VMEM((rows, width), jnp.bfloat16)],
        flops=4 * rows * depth * width,
    )
    remote_rows = max(8, (devices - 1) * CAP)
    local_bias, remote_bias = call(
        functools.partial(list_kernel, devices, turns),
        [chosen],
        [
            pltpu.VMEM((rows // BLOCK, rows), jnp.float32),
            pltpu.VMEM((remote_rows, rows), jnp.float32),
        ],
        scratch=[pltpu.VMEM(chosen.shape, chosen.dtype), pltpu.SemaphoreType.DMA],
        far=1,
    )
    state_shapes = [
        pltpu.VMEM((pairs, 2 * rows), jnp.float32),
        pltpu.VMEM((pairs, 2 * rows), jnp.float32),
        pltpu.VMEM((width, rows), jnp.float32),
    ]
    state = call(
        local_kernel, [queries, store, local_bias], state_shapes, flops=16 * rows * rows * width
    )
    for place in range(len(turns) - 1):
        state = call(
            functools.partial(remote_kernel, place, 0, False),
            [queries, remote_bias, got[place], *state],
            state_shapes,
            flops=16 * rows * CAP * BLOCK * width,
        )
    attended, swapped = [], []
    for part, (low, high) in enumerate(cuts):
        attended.append(
            call(
                functools.partial(remote_kernel, len(turns) - 1, low, True),
                [queries, remote_bias, got[len(turns) - 1 + part], *state],
                [pltpu.VMEM((rows, high - low), jnp.bfloat16)],
                flops=16 * rows * CAP * BLOCK * (high - low),
            )
        )
        swapped.append(lax.ppermute(attended[part], "tp", swap))
    out_width = out_weight.shape[1]
    part_shape = [pltpu.VMEM((rows, out_width), jnp.float32)]
    low = cuts[1][0]
    out_first = call(
        out_first_kernel,
        [attended[0], swapped[0], out_weight],
        part_shape,
        flops=4 * rows * low * out_width,
    )
    out_part = call(
        functools.partial(out_own_kernel, low),
        [out_first, attended[1], out_weight],
        part_shape,
        flops=2 * rows * (width - low) * out_width,
    )
    tiles = 4
    return call(
        functools.partial(out_kernel, low),
        [out_part, swapped[1], out_weight],
        [pltpu.HBM((rows, out_width), jnp.bfloat16)],
        flops=2 * rows * (width - low) * out_width,
        scratch=[
            pltpu.VMEM((tiles, rows, out_width // tiles), jnp.bfloat16),
            pltpu.SemaphoreType.DMA((tiles,)),
        ],
    )


def solution(mesh):
    placed = (
        P(("dp", "kv"), "tp"),
        P(None, "tp"),
        P(None, "tp"),
        P(None, "tp"),
        P(None, "tp"),
        P(("dp", "kv"), None),
    )
    return jax.shard_map(
        on_device, mesh=mesh, in_specs=placed, out_specs=P(("dp", "kv"), "tp"), check_vma=False
    )
```

```python
import functools

import jax
import jax.numpy as jnp
from jax import lax
from jax.experimental import pallas as pl
from jax.experimental.pallas import tpu as pltpu
from jax.sharding import PartitionSpec as P


HEAD_DIM = 64
BLOCK = 32
CAP = 3
LANES = 128

rotary_base = 500000.0
masked_score = -1e30
score_factor = HEAD_DIM ** (-0.5) * 1.4426950408889634


VMEM = pl.BlockSpec(memory_space=pltpu.VMEM)


def source_of(device, turn, devices):
    if devices & (devices - 1) == 0:
        return device ^ turn
    return (device + devices - turn) % devices


def turn_order(devices):
    last = devices - 1
    return [*range(2, last), *([1] if last > 1 else []), last]


def call(kernel, operands, results, flops=1000000, limit=16, scratch=(), far=0):
    anywhere = pl.BlockSpec(memory_space=pl.ANY)
    near = len(operands) - far
    out = pl.pallas_call(
        kernel,
        in_specs=[VMEM] * near + [anywhere] * far,
        out_specs=[anywhere if r.memory_space == pltpu.HBM else VMEM for r in results],
        out_shape=results,
        scratch_shapes=list(scratch),
        cost_estimate=pl.CostEstimate(flops=flops, bytes_accessed=100000, transcendentals=0),
        compiler_params=pltpu.CompilerParams(vmem_limit_bytes=limit << 20),
    )(
        *[pltpu.with_memory_space_constraint(x, pltpu.VMEM) for x in operands[:near]],
        *[pltpu.with_memory_space_constraint(x, pltpu.HBM) for x in operands[near:]],
    )
    return out[0] if len(results) == 1 else out


def dot(left, right):
    return jnp.dot(left, right, preferred_element_type=jnp.float32)


def table_kernel(cos_ref, sin_ref):
    rows = cos_ref.shape[0]
    half = HEAD_DIM // 2
    lane = lax.broadcasted_iota(jnp.int32, (BLOCK, LANES), 1) % half
    inverse = jnp.zeros((BLOCK, LANES), jnp.float32)
    for j in range(half):
        inverse = jnp.where(lane == j, float(1.0 / rotary_base ** (j / half)), inverse)
    offset = lax.broadcasted_iota(jnp.int32, (BLOCK, LANES), 0)
    start = lax.axis_index("kv") * rows + BLOCK * offset
    sign = jnp.where(
        lax.broadcasted_iota(jnp.int32, (BLOCK, LANES), 1) % HEAD_DIM < half, -1.0, 1.0
    )
    angle_in = offset.astype(jnp.float32) * inverse
    cos_in, sin_in = jnp.cos(angle_in), jnp.sin(angle_in)
    angle_at = start.astype(jnp.float32) * inverse
    cos_at, sin_at = jnp.cos(angle_at), jnp.sin(angle_at)
    for block in range(rows // BLOCK):
        at = slice(block * BLOCK, (block + 1) * BLOCK)
        cos_b, sin_b = cos_at[block : block + 1], sin_at[block : block + 1]
        cos_ref[at, :] = cos_in * cos_b - sin_in * sin_b
        sin_ref[at, :] = (sin_in * cos_b + cos_in * sin_b) * sign


def rotary_tables(rows):
    table = pltpu.VMEM((rows, LANES), jnp.float32)
    return call(table_kernel, [], [table] * 2, flops=2000000000)


def rotate(acc, cosine, sine):
    half = HEAD_DIM // 2
    lane = lax.broadcasted_iota(jnp.int32, (acc.shape[0], LANES), 1)
    first = lane % HEAD_DIM < half
    partner = jnp.where(first, pltpu.roll(acc, LANES - half, 1), pltpu.roll(acc, half, 1))
    return acc * cosine + partner * sine


def half_rows(weight_ref, other):
    mine = lax.axis_index("tp")
    depth = weight_ref.shape[0] // 2
    half = 1 - mine if other else mine
    return pl.ds(pl.multiple_of(half * depth, depth), depth)


def key_value_own_kernel(own_ref, key_ref, value_ref, out_ref):
    width = key_ref.shape[1]
    rows = half_rows(key_ref, False)
    out_ref[:, :width] = dot(own_ref[...], key_ref[rows, :])
    out_ref[:, width:] = dot(own_ref[...], value_ref[rows, :])


def key_value_kernel(part_ref, other_ref, key_ref, value_ref, cos_ref, sin_ref, out_ref):
    width = key_ref.shape[1]
    rows = half_rows(key_ref, True)
    key_acc = part_ref[:, :width] + dot(other_ref[...], key_ref[rows, :])
    cosine, sine = cos_ref[...], sin_ref[...]
    for start in range(0, width, LANES):
        lanes = slice(start, start + LANES)
        out_ref[:, lanes] = rotate(key_acc[:, lanes], cosine, sine).astype(jnp.bfloat16)
    value_acc = part_ref[:, width:] + dot(other_ref[...], value_ref[rows, :])
    out_ref[:, width:] = value_acc.astype(jnp.bfloat16)


def query_kernel(own_ref, other_ref, weight_ref, cos_ref, sin_ref, out_ref):
    acc = dot(own_ref[...], weight_ref[half_rows(weight_ref, False), :]) + dot(
        other_ref[...], weight_ref[half_rows(weight_ref, True), :]
    )
    cosine, sine = cos_ref[...], sin_ref[...]
    for start in range(0, acc.shape[1], LANES):
        lanes = slice(start, start + LANES)
        out_ref[:, lanes] = rotate(acc[:, lanes], cosine, sine).astype(jnp.bfloat16)


def pick_kernel(cuts, asked_ref, store_ref, *out_refs):
    blocks = store_ref.shape[0] // BLOCK
    width = store_ref.shape[1] // 2
    first = lax.axis_index("kv") * blocks
    asked = asked_ref[...]
    count = jnp.int32(0)
    index = [jnp.int32(0)] * CAP
    for block in range(blocks):
        hit = jnp.max((asked == first + block).astype(jnp.int32))
        for slot in range(CAP):
            index[slot] = jnp.where((hit == 1) & (count == slot), block, index[slot])
        count = count + hit
    for (low, high), out_ref in zip(cuts, out_refs):
        for slot in range(CAP):
            rows = pl.ds(pl.multiple_of(index[slot] * BLOCK, BLOCK), BLOCK)
            place = slice(slot * BLOCK, (slot + 1) * BLOCK)
            out_ref[place, : high - low] = store_ref[rows, low:high]
            out_ref[place, high - low :] = store_ref[rows, width + low : width + high]


def list_kernel(devices, turns, far_ref, local_ref, remote_ref, chosen_ref, sem):
    copy = pltpu.make_async_copy(far_ref, chosen_ref, sem)
    copy.start()
    copy.wait()
    blocks, slots = chosen_ref.shape
    rows = local_ref.shape[1]
    device = lax.axis_index("kv")
    spread = (
        lax.broadcasted_iota(jnp.int32, (blocks, rows), 1) // BLOCK
        == lax.broadcasted_iota(jnp.int32, (blocks, rows), 0)
    ).astype(jnp.float32)
    listed_ids = lax.dot_general(
        chosen_ref[...].astype(jnp.float32),
        spread,
        (((0,), (0,)), ((), ())),
        precision=lax.Precision.HIGHEST,
        preferred_element_type=jnp.float32,
    )
    row = lax.broadcasted_iota(jnp.int32, (blocks, rows), 0)
    for place, turn in enumerate([0, *turns]):
        source = source_of(device, turn, devices)
        ids = jnp.where(source <= device, source * blocks + row, -2).astype(jnp.float32)
        listed = jnp.zeros((blocks, rows), jnp.float32)
        for slot in range(slots):
            listed = jnp.where(listed_ids[slot : slot + 1, :] == ids, 1.0, listed)
        if turn == 0:
            local_ref[...] = jnp.where(listed > 0.0, 0.0, masked_score)
            continue
        needed = jnp.broadcast_to(jnp.max(listed, axis=1, keepdims=True), (blocks, rows))
        rank, step = needed, 1
        while step < blocks:
            rank = rank + jnp.where(row >= step, pltpu.roll(rank, step, 0), 0.0)
            step *= 2
        for slot in range(CAP):
            here = jnp.where((needed > 0.0) & (rank == slot + 1.0), listed, 0.0)
            hit = jnp.max(here, axis=0, keepdims=True)
            at = (place - 1) * CAP + slot
            remote_ref[at : at + 1, :] = jnp.where(hit > 0.0, 0.0, masked_score)


def head_pair_queries(queries):
    lane = lax.broadcasted_iota(jnp.int32, queries.shape, 1)
    zero = jnp.zeros_like(queries)
    return jnp.concatenate(
        [jnp.where(lane < HEAD_DIM, queries, zero), jnp.where(lane < HEAD_DIM, zero, queries)],
        axis=0,
    )


def pair_scores(keys, queries):
    return lax.dot_general(
        keys, queries, (((1,), (1,)), ((), ())), preferred_element_type=jnp.float32
    )


def pair_values(values, weights):
    both = lax.dot_general(
        values, weights, (((0,), (0,)), ((), ())), preferred_element_type=jnp.float32
    )
    rows = weights.shape[1] // 2
    return jnp.concatenate([both[:HEAD_DIM, :rows], both[HEAD_DIM:, rows:]], axis=0)


def widen(stat):
    rows = stat.shape[1] // 2
    return jnp.concatenate(
        [
            jnp.broadcast_to(stat[:, :rows], (HEAD_DIM, rows)),
            jnp.broadcast_to(stat[:, rows:], (HEAD_DIM, rows)),
        ],
        axis=0,
    )


def local_kernel(query_ref, store_ref, bias_ref, peak_ref, total_ref, summed_ref):
    rows, width = query_ref.shape
    blocks = rows // BLOCK
    listed = jnp.concatenate(
        [jnp.broadcast_to(bias_ref[b : b + 1, :], (BLOCK, rows)) for b in range(blocks)], axis=0
    )
    key_row = lax.broadcasted_iota(jnp.int32, (rows, rows), 0)
    query_row = lax.broadcasted_iota(jnp.int32, (rows, rows), 1)
    bias = jnp.where(key_row <= query_row, listed, masked_score)
    bias = jnp.concatenate([bias, bias], axis=1)
    for pair in range(width // LANES):
        lanes = slice(pair * LANES, (pair + 1) * LANES)
        queries = head_pair_queries(query_ref[:, lanes])
        scores = pair_scores(store_ref[:, lanes], queries) + bias
        peak = jnp.max(scores, axis=0, keepdims=True)
        weights = jnp.exp2((scores - peak) * score_factor)
        peak_ref[pair : pair + 1, :] = peak
        total_ref[pair : pair + 1, :] = jnp.sum(weights, axis=0, keepdims=True)
        values = store_ref[:, width + pair * LANES : width + (pair + 1) * LANES]
        summed_ref[lanes, :] = pair_values(values, weights.astype(jnp.bfloat16))


def remote_kernel(place, low, last, query_ref, bias_ref, got_ref, *refs):
    (peak_ref, total_ref, summed_ref), out_refs = refs[:3], refs[3:]
    rows = query_ref.shape[0]
    width = got_ref.shape[1] // 2
    count = width // LANES
    bias = jnp.concatenate(
        [
            jnp.broadcast_to(bias_ref[s : s + 1, :], (BLOCK, rows))
            for s in range(place * CAP, (place + 1) * CAP)
        ],
        axis=0,
    )
    bias = jnp.concatenate([bias, bias], axis=1)
    here = [slice(p * LANES, (p + 1) * LANES) for p in range(count)]
    lanes = [slice(low + h.start, low + h.stop) for h in here]
    stats = [low // LANES + p for p in range(count)]
    scores = [
        pair_scores(got_ref[:, here[p]], head_pair_queries(query_ref[:, lanes[p]])) + bias
        for p in range(count)
    ]
    weights, factors, totals = [], [], []
    for p, at in enumerate(stats):
        peak = peak_ref[at : at + 1, :]
        peak_new = jnp.maximum(peak, jnp.max(scores[p], axis=0, keepdims=True))
        factor = jnp.exp2((peak - peak_new) * score_factor)
        weight = jnp.exp2((scores[p] - peak_new) * score_factor)
        total = total_ref[at : at + 1, :] * factor + jnp.sum(weight, axis=0, keepdims=True)
        weights.append(weight.astype(jnp.bfloat16))
        factors.append(factor)
        totals.append(total)
        if not last:
            out_refs[0][at : at + 1, :] = peak_new
            out_refs[1][at : at + 1, :] = total
    added = [
        pair_values(got_ref[:, width + here[p].start : width + here[p].stop], weights[p])
        for p in range(count)
    ]
    for p in range(count):
        if last:
            over = 1.0 / totals[p]
            summed = summed_ref[lanes[p], :] * widen(factors[p] * over) + added[p] * widen(over)
            out_refs[0][:, here[p]] = summed.T.astype(jnp.bfloat16)
        else:
            out_refs[2][lanes[p], :] = summed_ref[lanes[p], :] * widen(factors[p]) + added[p]


def head_rows(weight_ref, other, low, width):
    mine = lax.axis_index("tp")
    depth = weight_ref.shape[0] // 2
    half = 1 - mine if other else mine
    return pl.ds(pl.multiple_of(half * depth + low, LANES), width)


def out_first_kernel(own_ref, other_ref, weight_ref, out_ref):
    width = own_ref.shape[1]
    out_ref[...] = dot(own_ref[...], weight_ref[head_rows(weight_ref, False, 0, width), :]) + dot(
        other_ref[...], weight_ref[head_rows(weight_ref, True, 0, width), :]
    )


def out_own_kernel(low, part_ref, own_ref, weight_ref, out_ref):
    rows = head_rows(weight_ref, False, low, own_ref.shape[1])
    out_ref[...] = part_ref[...] + dot(own_ref[...], weight_ref[rows, :])


def out_kernel(low, part_ref, other_ref, weight_ref, out_ref, tile_ref, sems):
    tiles = tile_ref.shape[0]
    width = tile_ref.shape[2]
    rows = head_rows(weight_ref, True, low, other_ref.shape[1])
    copies = []
    for tile in range(tiles):
        lanes = slice(tile * width, (tile + 1) * width)
        acc = part_ref[:, lanes] + dot(other_ref[...], weight_ref[rows, lanes])
        tile_ref[tile] = acc.astype(jnp.bfloat16)
        copies.append(
            pltpu.make_async_copy(tile_ref.at[tile], out_ref.at[:, lanes], sems.at[tile])
        )
        copies[-1].start()
    for copy in copies:
        copy.wait()


def on_device(tokens, query_weight, key_weight, value_weight, out_weight, chosen):
    rows, depth = tokens.shape
    width = query_weight.shape[1]
    pairs = width // LANES
    devices = lax.axis_size("kv")
    swap = [(0, 1), (1, 0)]

    def ask(x, turn):
        return lax.ppermute(x, "kv", [(i, source_of(i, turn, devices)) for i in range(devices)])

    def send(x, turn):
        pairs = [(source_of(i, turn, devices), i) for i in range(devices)]
        if turn == turns[-1]:
            pairs = [pair for pair in pairs if pair[0] < pair[1]]
        return lax.ppermute(x, "kv", pairs)

    other = lax.ppermute(tokens, "tp", swap)
    asked, turns = [], turn_order(devices)
    for turn in turns:
        asked.append(ask(chosen, turn))
    cosine, sine = rotary_tables(rows)
    part = call(
        key_value_own_kernel,
        [tokens, key_weight, value_weight],
        [pltpu.VMEM((rows, 2 * width), jnp.float32)],
        flops=4 * rows * depth * width,
    )
    store = call(
        key_value_kernel,
        [part, other, key_weight, value_weight, cosine, sine],
        [pltpu.VMEM((rows, 2 * width), jnp.bfloat16)],
        flops=4 * rows * depth * width,
    )
    cut = width // 2
    cuts = [(0, cut), (cut, width)]
    got = []
    for turn, asked_by in zip(turns, asked):
        parts = cuts if turn == turns[-1] else [(0, width)]
        picked = call(
            functools.partial(pick_kernel, parts),
            [asked_by, store],
            [pltpu.VMEM((CAP * BLOCK, 2 * (high - low)), jnp.bfloat16) for low, high in parts],
        )
        for part, block in enumerate(picked if len(parts) > 1 else [picked]):
            got.append(send(block, turn))
    queries = call(
        query_kernel,
        [tokens, other, query_weight, cosine, sine],
        [pltpu.VMEM((rows, width), jnp.bfloat16)],
        flops=4 * rows * depth * width,
    )
    remote_rows = max(8, (devices - 1) * CAP)
    local_bias, remote_bias = call(
        functools.partial(list_kernel, devices, turns),
        [chosen],
        [
            pltpu.VMEM((rows // BLOCK, rows), jnp.float32),
            pltpu.VMEM((remote_rows, rows), jnp.float32),
        ],
        scratch=[pltpu.VMEM(chosen.shape, chosen.dtype), pltpu.SemaphoreType.DMA],
        far=1,
    )
    state_shapes = [
        pltpu.VMEM((pairs, 2 * rows), jnp.float32),
        pltpu.VMEM((pairs, 2 * rows), jnp.float32),
        pltpu.VMEM((width, rows), jnp.float32),
    ]
    state = call(
        local_kernel, [queries, store, local_bias], state_shapes, flops=16 * rows * rows * width
    )
    for place in range(len(turns) - 1):
        state = call(
            functools.partial(remote_kernel, place, 0, False),
            [queries, remote_bias, got[place], *state],
            state_shapes,
            flops=16 * rows * CAP * BLOCK * width,
        )
    attended, swapped = [], []
    for part, (low, high) in enumerate(cuts):
        attended.append(
            call(
                functools.partial(remote_kernel, len(turns) - 1, low, True),
                [queries, remote_bias, got[len(turns) - 1 + part], *state],
                [pltpu.VMEM((rows, high - low), jnp.bfloat16)],
                flops=16 * rows * CAP * BLOCK * (high - low),
            )
        )
        swapped.append(lax.ppermute(attended[part], "tp", swap))
    out_width = out_weight.shape[1]
    part_shape = [pltpu.VMEM((rows, out_width), jnp.float32)]
    low = cuts[1][0]
    out_first = call(
        out_first_kernel,
        [attended[0], swapped[0], out_weight],
        part_shape,
        flops=4 * rows * low * out_width,
    )
    out_part = call(
        functools.partial(out_own_kernel, low),
        [out_first, attended[1], out_weight],
        part_shape,
        flops=2 * rows * (width - low) * out_width,
    )
    tiles = 4
    return call(
        functools.partial(out_kernel, low),
        [out_part, swapped[1], out_weight],
        [pltpu.HBM((rows, out_width), jnp.bfloat16)],
        flops=2 * rows * (width - low) * out_width,
        scratch=[
            pltpu.VMEM((tiles, rows, out_width // tiles), jnp.bfloat16),
            pltpu.SemaphoreType.DMA((tiles,)),
        ],
    )


def solution(mesh):
    placed = (
        P(("dp", "kv"), "tp"),
        P(None, "tp"),
        P(None, "tp"),
        P(None, "tp"),
        P(None, "tp"),
        P(("dp", "kv"), None),
    )
    return jax.shard_map(
        on_device, mesh=mesh, in_specs=placed, out_specs=P(("dp", "kv"), "tp"), check_vma=False
    )
```
